32 devices in a mesh: sp: 8 (over z, x), tp: 4 (over y, core).
Axes of the slice: x: 2, y: 2, z: 4, core: 2. Of those that a mesh axis runs over, the one named last changes fastest.
Arguments:
- queries: bfloat16 [5120, 1024], P('sp', 'tp'), may hold values from -6 to 6
- key_head_rows: bfloat16 [5120, 1024], P('sp', 'tp'), may hold values from -6 to 6
- value_head_rows: bfloat16 [5120, 2048], P('sp', 'tp'), may hold values from -6 to 6
- output_gate_preact: bfloat16 [5120, 2048], P('sp', 'tp'), may hold values from -6 to 6
- log_input_gate: float32 [16, 5120], P('tp', 'sp'), may hold values from -4 to 300
- forget_gate_preact: float32 [16, 5120], P('tp', 'sp')
- extra_log_decay: float32 [16, 5120], P('tp', 'sp'), may hold values from -2.1 to 0
- head_norm_gain: float32 [2048], P('tp'), may hold values from 0.1 to 1.9
- residual: bfloat16 [5120, 2048], P(('sp', 'tp')), may hold values from -6 to 6
- cell_output_weight: bfloat16 [2048, 2048], P('tp'), may hold values from -0.25 to 0.25
- feedforward_norm_gain: float32 [2048], replicated, may hold values from 0.1 to 1.9
- gate_projection_weight: bfloat16 [2048, 5632], P('sp', 'tp'), may hold values from -0.125 to 0.125
- up_projection_weight: bfloat16 [2048, 5632], P('sp', 'tp'), may hold values from -0.125 to 0.125
- down_projection_weight: bfloat16 [5632, 2048], P('tp', 'sp'), may hold values from -0.109375 to 0.109375
Outputs:
- layer_out: bfloat16 [5120, 2048], P(('sp', 'tp'))
The draws below stay inside these ranges and needn't reach their ends.
All inputs are finite; a program needn't handle non-finite values.
Results may differ from the reference program's by a relative error of at most 0.015.
Values may be sent and summed in bfloat16 or wider, within the bound.
A program may use at most 128 MiB of HBM per device.

```python
import jax
import jax.numpy as jnp
from jax import lax

D = 2048
HEADS = 16
DQK = 64
DV = 128
FF = 5632
BLOCK = 128
TOK_DEV = 640
TOKENS = 5120
HV = 2048
N_TP = 4


def draw_log_input_gate(key, part):
    base_key = jax.random.fold_in(key, 0)
    return jnp.clip(jax.random.normal(base_key, (HEADS, TOKENS), jnp.float32), -4.0, 4.0)


def draw_forget_gate_preact(key, part):
    kind_key, block_key, noise_key = jax.random.split(key, 3)
    fast_share = 0.5
    fast_heads = jax.random.uniform(kind_key, (HEADS, 1), jnp.float32) < fast_share
    base_rate = jnp.where(fast_heads, 1.0 / 40.0, 0.5 / TOKENS)
    span_scale = jax.random.uniform(block_key, (HEADS, TOKENS // TOK_DEV), jnp.float32, 0.35, 1.0)
    span_scale = jnp.repeat(span_scale, TOK_DEV, axis=1)
    jitter = jnp.exp(0.7 * jnp.clip(jax.random.normal(noise_key, (HEADS, TOKENS), jnp.float32), -3.0, 3.0))
    decay_rate = base_rate * span_scale * jitter
    return -jnp.log(jnp.expm1(decay_rate))


def draw_extra_log_decay(key, part):
    spot_key, size_key = jax.random.split(key, 2)
    spot_list = jax.random.randint(spot_key, (HEADS, 3), 0, TOKENS)
    drop_sizes = jax.random.uniform(size_key, (HEADS, 3, 1), jnp.float32, 0.22, 0.69)
    hit_mask = jnp.arange(TOKENS)[None, None, :] == spot_list[:, :, None]
    return -jnp.sum(jnp.where(hit_mask, drop_sizes, 0.0), axis=1)


def block_scale(key, shape, shards, least, top_value):
    def one(dim, parts):
        draws = jax.random.uniform(jax.random.fold_in(jax.random.fold_in(key, 6), dim), (parts,), jnp.float32, least / len(shards), top_value / len(shards))
        return jnp.repeat(jnp.exp(draws), shape[dim] // parts).reshape((-1,) + (1,) * (len(shape) - dim - 1))

    factor_of = one(*shards[0])
    for cut in shards[1:]:
        factor_of = factor_of * one(*cut)
    return factor_of


def noise(own_key, shape, scale, most, cuts=(), dtype=jnp.bfloat16):
    result = scale * jax.random.normal(own_key, shape, jnp.float32)
    if cuts:
        result = result * block_scale(own_key, shape, cuts, -0.22, 0.18)
    return jnp.clip(result, -most, most).astype(dtype)


def setup_inputs(seed: int = 0) -> dict:
    key_of = jax.random.split(jax.random.key(seed), 15)
    queries = noise(key_of[0], (TOKENS, HEADS * DQK), 1.0, 6.0, ((0, 8), (1, 4)))
    key_head_rows = noise(key_of[1], (TOKENS, HEADS * DQK), 1.0, 6.0, ((0, 8), (1, 4)))
    value_head_rows = noise(key_of[2], (TOKENS, HV), 1.0, 6.0, ((0, 8), (1, 4)))
    output_gate_preact = noise(key_of[3], (TOKENS, HV), 1.0, 6.0, ((0, 8), (1, 4)))
    log_input_gate = draw_log_input_gate(jax.random.fold_in(key_of[14], 71), 0)
    forget_gate_preact = draw_forget_gate_preact(jax.random.fold_in(key_of[14], 71), 0)
    extra_log_decay = draw_extra_log_decay(jax.random.fold_in(key_of[14], 71), 0)
    head_norm_gain = jnp.clip(1.0 + 0.18 * jax.random.normal(key_of[7], (HV,), jnp.float32), 0.1, 1.9)
    residual = noise(key_of[8], (TOKENS, D), 1.0, 6.0, ((0, 32),))
    cell_output_weight = noise(key_of[9], (HV, D), (HV // 4) ** -0.5, 0.25, ((0, 4),))
    feedforward_norm_gain = jnp.clip(1.0 + 0.18 * jax.random.normal(key_of[10], (D,), jnp.float32), 0.1, 1.9)
    gate_projection_weight = noise(key_of[11], (D, FF), D ** -0.5, 0.125, ((0, 8), (1, 4)))
    up_projection_weight = noise(key_of[12], (D, FF), D ** -0.5, 0.125, ((0, 8), (1, 4)))
    down_projection_weight = noise(key_of[13], (FF, D), (FF // 2) ** -0.5, 0.109375, ((0, 4), (1, 8)))
    return {"queries": queries, "key_head_rows": key_head_rows, "value_head_rows": value_head_rows, "output_gate_preact": output_gate_preact, "log_input_gate": log_input_gate, "forget_gate_preact": forget_gate_preact, "extra_log_decay": extra_log_decay, "head_norm_gain": head_norm_gain, "residual": residual, "cell_output_weight": cell_output_weight, "feedforward_norm_gain": feedforward_norm_gain, "gate_projection_weight": gate_projection_weight, "up_projection_weight": up_projection_weight, "down_projection_weight": down_projection_weight}


epsilon = 1e-06
lowest = -1e+30

def merge_states(earlier, later):
    state_one, top_one, total_one = earlier
    state_two, top_two, total_two = later
    top_new = jnp.maximum(total_two + top_one, top_two)
    scale_one = jnp.exp(total_two + top_one - top_new)
    scale_two = jnp.exp(top_two - top_new)
    state_new = scale_one[..., None, None] * state_one + scale_two[..., None, None] * state_two
    return (state_new, top_new, total_one + total_two)

def block_parts(key_block, value_block, gate_block, forget_block):
    running = jnp.cumsum(forget_block, axis=-1)
    totals = running[..., -1]
    to_end = totals[..., None] - running + gate_block
    top_block = lax.optimization_barrier(jnp.max(to_end, axis=-1))
    factor = jnp.exp(to_end - top_block[..., None]) * DQK ** (-0.5)
    weighted = (key_block.astype(jnp.float32) * factor[..., None]).astype(jnp.bfloat16)
    states = jnp.einsum('nhsd,nhse->nhde', weighted.astype(jnp.float32), value_block.astype(jnp.float32))
    return (running, (states, top_block, totals))

def block_output(query_block, key_block, value_block, gate_block, running, carried_state, carried_top):
    length = query_block.shape[-2]
    scores = jnp.einsum('nhtd,nhsd->nhts', query_block.astype(jnp.float32), key_block.astype(jnp.float32)) * DQK ** (-0.5)
    log_decay = running[..., :, None] - running[..., None, :] + gate_block[..., None, :]
    causal = jnp.arange(length)[:, None] >= jnp.arange(length)[None, :]
    log_decay = jnp.where(causal, log_decay, -jnp.inf)
    carried = running + carried_top[..., None]
    row_top = jnp.maximum(carried, lax.optimization_barrier(jnp.max(log_decay, axis=-1)))
    weights = (scores * jnp.exp(log_decay - row_top[..., None])).astype(jnp.bfloat16)
    within = jnp.einsum('nhts,nhse->nhte', weights.astype(jnp.float32), value_block.astype(jnp.float32))
    across = jnp.einsum('nhtd,nhde->nhte', query_block.astype(jnp.float32), carried_state, precision=lax.Precision.HIGHEST)
    return jnp.exp(carried - row_top)[..., None] * across + within

def grouped_product(left, right, groups):
    columns = left.shape[1] // groups
    summed = jnp.zeros((left.shape[0], right.shape[1]), jnp.float32)
    for member in range(groups):
        product = jnp.dot(left[:, member * columns:(member + 1) * columns], right[member * columns:(member + 1) * columns], preferred_element_type=jnp.float32)
        rounded = lax.optimization_barrier(product.astype(jnp.bfloat16))
        summed = summed + rounded.astype(jnp.float32)
    return summed

def reference(queries, key_head_rows, value_head_rows, output_gate_preact, log_input_gate, forget_gate_preact, extra_log_decay, head_norm_gain, residual, cell_output_weight, feedforward_norm_gain, gate_projection_weight, up_projection_weight, down_projection_weight):
    blocks = TOKENS // BLOCK

    def split_heads(matrix, head_size):
        return matrix.reshape(blocks, BLOCK, HEADS, head_size).transpose(0, 2, 1, 3)

    def split_gate_parts(gates):
        return gates.reshape(HEADS, blocks, BLOCK).transpose(1, 0, 2)
    log_forget_gate = jax.nn.log_sigmoid(forget_gate_preact) + extra_log_decay
    inputs = (split_heads(queries, DQK), split_heads(key_head_rows, DQK), split_heads(value_head_rows, DV), split_gate_parts(log_input_gate), split_gate_parts(log_forget_gate))

    def advance(history, segment):
        query_block, key_block, value_block, gate_block, forget_block = [member[None] for member in segment]
        running, summary = block_parts(key_block, value_block, gate_block, forget_block)
        numerator = block_output(query_block, key_block, value_block, gate_block, running, history[0][None], history[1][None])
        history = merge_states(history, tuple((member[0] for member in summary)))
        return (history, numerator[0])
    initial = (jnp.zeros((HEADS, DQK, DV), jnp.float32), jnp.full((HEADS,), lowest, jnp.float32), jnp.zeros((HEADS,), jnp.float32))
    _, numerators = lax.scan(advance, initial, inputs)
    numerators = numerators.transpose(0, 2, 1, 3).reshape(TOKENS, HEADS, DV)
    normalized = numerators * lax.rsqrt(lax.optimization_barrier(jnp.mean(numerators * numerators, axis=-1, keepdims=True)) + epsilon)
    cell_rows = (normalized.reshape(TOKENS, HV) * head_norm_gain * jax.nn.sigmoid(output_gate_preact.astype(jnp.float32))).astype(jnp.bfloat16)

    def finish(segment):
        cell_block, residual_block = segment
        mixed_rows = (residual_block.astype(jnp.float32) + grouped_product(cell_block, cell_output_weight, N_TP)).astype(jnp.bfloat16)
        mixed_float = mixed_rows.astype(jnp.float32)
        normed = (mixed_float * lax.rsqrt(lax.optimization_barrier(jnp.mean(mixed_float * mixed_float, axis=-1, keepdims=True)) + epsilon) * feedforward_norm_gain).astype(jnp.bfloat16)
        gate_proj = jnp.dot(normed, gate_projection_weight, preferred_element_type=jnp.float32)
        up_proj = jnp.dot(normed, up_projection_weight, preferred_element_type=jnp.float32)
        hidden = (jax.nn.silu(gate_proj) * up_proj).astype(jnp.bfloat16)
        return (mixed_float + grouped_product(hidden, down_projection_weight, N_TP)).astype(jnp.bfloat16)
    outputs = lax.map(finish, (cell_rows.reshape(TOKENS // TOK_DEV, TOK_DEV, HV), residual.reshape(TOKENS // TOK_DEV, TOK_DEV, D)))
    return outputs.reshape(TOKENS, D)
```

```python
import jax
import jax.numpy as jnp
from jax import lax
from jax.sharding import PartitionSpec as P

DQK = 64
DV = 128
BLOCK = 128


epsilon = 1e-06
lowest = -1e30


def swap(value, axis, bit):
    return lax.ppermute(value, axis, [(i, i ^ bit) for i in range(lax.axis_size(axis))])


def bits_below(size):
    return [1 << k for k in range(size.bit_length() - 1)]


def pack_state(state):
    value, top, total = state
    heads, _, width = value.shape
    extra = jnp.stack([top, total], axis=1)[:, :, None]
    extra = jnp.broadcast_to(extra, (heads, 2, width))
    return jnp.concatenate([value, extra, jnp.zeros((heads, 6, width), jnp.float32)], axis=1)


def unpack_state(packed):
    depth = packed.shape[1] - 8
    return (packed[:, :depth], packed[:, depth, 0], packed[:, depth + 1, 0])


def choose(condition, first, second):
    return jax.tree.map(lambda a, b: jnp.where(condition, a, b), first, second)


def prefix_of(state, axis, blank):
    here = lax.axis_index(axis)
    before, whole = blank, state
    for bit in bits_below(lax.axis_size(axis)):
        other = unpack_state(swap(pack_state(whole), axis, bit))
        upper = (here & bit) != 0
        before = choose(upper, merge_states(other, before), before)
        whole = merge_states(choose(upper, other, whole), choose(upper, whole, other))
    return before


def spread(piece, bits):
    held = [(0, piece)]
    for bit in bits:
        held = held + [(mask | bit, swap(value, "sp", bit)) for mask, value in held]
    return held


def merge_states(earlier, later):
    state_one, top_one, total_one = earlier
    state_two, top_two, total_two = later
    top_new = jnp.maximum(total_two + top_one, top_two)
    scale_one = jnp.exp(total_two + top_one - top_new)
    scale_two = jnp.exp(top_two - top_new)
    state_new = scale_one[..., None, None] * state_one + scale_two[..., None, None] * state_two
    return (state_new, top_new, total_one + total_two)


def block_parts(key_block, value_block, gate_block, forget_block):
    running = jnp.cumsum(forget_block, axis=-1)
    totals = running[..., -1]
    to_end = totals[..., None] - running + gate_block
    top_block = jnp.max(to_end, axis=-1)
    factor = jnp.exp(to_end - top_block[..., None]) * DQK ** (-0.5)
    weighted = (key_block * factor[..., None]).astype(jnp.bfloat16)
    states = jnp.einsum(
        "nhsd,nhse->nhde", weighted, value_block, preferred_element_type=jnp.float32
    )
    return (running, (states, top_block, totals))


def block_output(
    query_block, key_block, value_block, gate_block, running, carried_state, carried_top
):
    length = query_block.shape[-2]
    scores = jnp.einsum(
        "nhtd,nhsd->nhts", query_block, key_block, preferred_element_type=jnp.float32
    ) * DQK ** (-0.5)
    log_decay = running[..., :, None] - running[..., None, :] + gate_block[..., None, :]
    causal = jnp.arange(length)[:, None] >= jnp.arange(length)[None, :]
    log_decay = jnp.where(causal, log_decay, -jnp.inf)
    carried = running + carried_top[..., None]
    row_top = jnp.maximum(carried, jnp.max(log_decay, axis=-1))
    weights = (scores * jnp.exp(log_decay - row_top[..., None])).astype(jnp.bfloat16)
    within = jnp.einsum("nhts,nhse->nhte", weights, value_block, preferred_element_type=jnp.float32)
    across = jnp.einsum(
        "nhtd,nhde->nhte",
        query_block.astype(jnp.float32),
        carried_state,
        precision=lax.Precision.HIGHEST,
    )
    return jnp.exp(carried - row_top)[..., None] * across + within


def per_device(
    queries,
    key_head_rows,
    value_head_rows,
    output_gate_preact,
    log_input_gate,
    forget_gate_preact,
    extra_log_decay,
    head_norm_gain,
    residual,
    cell_output_weight,
    feedforward_norm_gain,
    gate_projection_weight,
    up_projection_weight,
    down_projection_weight,
):
    size = lax.axis_size("sp")
    here = lax.axis_index("sp")
    place = lax.axis_index("tp")
    tp_bits = bits_below(lax.axis_size("tp"))
    sp_bits = bits_below(size)
    share = sp_bits[len(sp_bits) // 2]
    others = [bit for bit in reversed(sp_bits) if bit != share]
    half = gate_projection_weight.shape[1] // 2
    upper = (here & share) != 0

    def halves(first, second):
        return jnp.where(upper, second, first), jnp.where(upper, first, second)

    def columns_of(weight):
        mine, theirs = halves(weight[:, :half], weight[:, half:])
        return jnp.concatenate([mine, swap(theirs, "sp", share)], axis=0)

    def rows_of(weight):
        mine, theirs = halves(weight[:half], weight[half:])
        return jnp.concatenate([mine, swap(theirs, "sp", share)], axis=1)

    gate_pair = columns_of(gate_projection_weight)
    up_pair = columns_of(up_projection_weight)
    down_pair = rows_of(down_projection_weight)
    gate_pieces = spread(gate_pair, others)
    tokens_here = queries.shape[0]
    heads_here = queries.shape[1] // DQK
    blocks = tokens_here // BLOCK

    def split_heads(matrix, head_size):
        return matrix.reshape(blocks, BLOCK, heads_here, head_size).transpose(0, 2, 1, 3)

    def split_gate_parts(gates):
        return gates.reshape(heads_here, blocks, BLOCK).transpose(1, 0, 2)

    query_blocks = split_heads(queries, DQK)
    key_blocks = split_heads(key_head_rows, DQK)
    value_blocks = split_heads(value_head_rows, DV)
    gate_blocks = split_gate_parts(log_input_gate)
    forget_gate_blocks = split_gate_parts(jax.nn.log_sigmoid(forget_gate_preact) + extra_log_decay)
    running, summary = block_parts(key_blocks, value_blocks, gate_blocks, forget_gate_blocks)
    blank_state = (
        jnp.zeros((heads_here, DQK, DV), jnp.float32),
        jnp.full((heads_here,), lowest, jnp.float32),
        jnp.zeros((heads_here,), jnp.float32),
    )
    device_state = blank_state
    prefixes = []
    for position in range(blocks):
        prefixes.append(device_state)
        device_state = merge_states(device_state, tuple((member[position] for member in summary)))
    incoming = prefix_of(device_state, "sp", blank_state)
    incoming, up_pair, down_pair = lax.optimization_barrier((incoming, up_pair, down_pair))
    up_pieces = spread(up_pair, others)
    down_pieces = spread(down_pair, others)
    stacked = tuple(jnp.stack(member) for member in zip(*prefixes))
    carried_state, carried_top, _ = merge_states(
        tuple(member[None] for member in incoming), stacked
    )
    numerators = block_output(
        query_blocks, key_blocks, value_blocks, gate_blocks, running, carried_state, carried_top
    )
    numerators = numerators.transpose(0, 2, 1, 3).reshape(tokens_here, heads_here, DV)
    normalized = numerators * lax.rsqrt(
        jnp.mean(numerators * numerators, axis=-1, keepdims=True) + epsilon
    )
    cell_rows = (
        normalized.reshape(tokens_here, heads_here * DV)
        * head_norm_gain
        * jax.nn.sigmoid(output_gate_preact.astype(jnp.float32))
    ).astype(jnp.bfloat16)
    tp_size = lax.axis_size("tp")
    rows = tokens_here // tp_size
    flips = list(reversed(tp_bits))
    order = [0]
    for bit in flips:
        order = order + [mask | bit for mask in order]
    ordered = jnp.concatenate(
        [
            lax.dynamic_slice_in_dim(cell_rows, (place ^ mask) * rows, rows, 0)
            for mask in order
        ],
        axis=0,
    )
    projected = jnp.dot(ordered, cell_output_weight, preferred_element_type=jnp.float32).astype(
        jnp.bfloat16
    )

    def sum_over_tp(parts):
        for bit in tp_bits:
            kept, sent = jnp.split(parts.astype(jnp.bfloat16), 2, axis=0)
            parts = kept.astype(jnp.float32) + swap(sent, "tp", bit).astype(jnp.float32)
        return parts

    mixed_float = (
        (residual.astype(jnp.float32) + sum_over_tp(projected))
        .astype(jnp.bfloat16)
        .astype(jnp.float32)
    )
    normed = (
        mixed_float
        * lax.rsqrt(jnp.mean(mixed_float * mixed_float, axis=-1, keepdims=True) + epsilon)
        * feedforward_norm_gain
    ).astype(jnp.bfloat16)

    held = [normed, swap(normed, "sp", share)]
    for bit in flips[:-1]:
        held = held + [swap(value, "tp", bit) for value in held]
    near = jnp.concatenate(held, axis=0)
    all_rows = jnp.concatenate([near, swap(near, "tp", flips[-1])], axis=0)

    width = gate_projection_weight.shape[0]
    masks = [mask | low for mask, _ in gate_pieces for low in (0, share)]
    all_rows = jnp.concatenate(
        [lax.dynamic_slice_in_dim(all_rows, (here ^ mask) * width, width, 1) for mask in masks],
        axis=1,
    )
    whole_gate = jnp.concatenate([value for _, value in gate_pieces], axis=0)
    whole_up = jnp.concatenate([value for _, value in up_pieces], axis=0)
    gate_proj = jnp.dot(all_rows, whole_gate, preferred_element_type=jnp.float32)
    up_proj = jnp.dot(all_rows, whole_up, preferred_element_type=jnp.float32)
    hidden = (jax.nn.silu(gate_proj) * up_proj).astype(jnp.bfloat16)

    summed = {}
    for mask, value in down_pieces:
        partial = jnp.dot(hidden, value, preferred_element_type=jnp.float32)
        partial = sum_over_tp(partial).astype(jnp.bfloat16)
        kept, sent = partial[:rows], partial[rows:]
        turned = jnp.concatenate([sent[:, width:], sent[:, :width]], axis=1)
        total = kept.astype(jnp.float32) + swap(turned, "sp", share).astype(jnp.float32)
        summed[mask], summed[mask | share] = total[:, :width], total[:, width:]
    relative = jnp.concatenate([summed[mask] for mask in range(size)], axis=1)
    summed = jnp.concatenate(
        [
            lax.dynamic_slice_in_dim(relative, (here ^ block) * width, width, 1)
            for block in range(size)
        ],
        axis=1,
    )
    return (mixed_float + summed).astype(jnp.bfloat16)


def solution(mesh):
    placed = (
        P("sp", "tp"),
        P("sp", "tp"),
        P("sp", "tp"),
        P("sp", "tp"),
        P("tp", "sp"),
        P("tp", "sp"),
        P("tp", "sp"),
        P("tp"),
        P(("sp", "tp"), None),
        P("tp", None),
        P(),
        P("sp", "tp"),
        P("sp", "tp"),
        P("tp", "sp"),
    )
    return jax.shard_map(
        per_device, mesh=mesh, in_specs=placed, out_specs=P(("sp", "tp"), None), check_vma=False
    )
```

```python
import jax
import jax.numpy as jnp
from jax import lax
from jax.sharding import PartitionSpec as P


DQK = 64
DV = 128
BLOCK = 128


epsilon = 1e-06
lowest = -1e30


def swap(value, axis, bit):
    return lax.ppermute(value, axis, [(i, i ^ bit) for i in range(lax.axis_size(axis))])


def bits_below(size):
    return [1 << k for k in range(size.bit_length() - 1)]


def pack_state(state):
    value, top, total = state
    heads, _, width = value.shape
    extra = jnp.stack([top, total], axis=1)[:, :, None]
    extra = jnp.broadcast_to(extra, (heads, 2, width))
    return jnp.concatenate([value, extra, jnp.zeros((heads, 6, width), jnp.float32)], axis=1)


def unpack_state(packed):
    depth = packed.shape[1] - 8
    return (packed[:, :depth], packed[:, depth, 0], packed[:, depth + 1, 0])


def choose(condition, first, second):
    return jax.tree.map(lambda a, b: jnp.where(condition, a, b), first, second)


def prefix_of(state, axis, blank):
    here = lax.axis_index(axis)
    before, whole = blank, state
    for bit in bits_below(lax.axis_size(axis)):
        other = unpack_state(swap(pack_state(whole), axis, bit))
        upper = (here & bit) != 0
        before = choose(upper, merge_states(other, before), before)
        whole = merge_states(choose(upper, other, whole), choose(upper, whole, other))
    return before


def spread(piece, bits):
    held = [(0, piece)]
    for bit in bits:
        held = held + [(mask | bit, swap(value, "sp", bit)) for mask, value in held]
    return held


def merge_states(earlier, later):
    state_one, top_one, total_one = earlier
    state_two, top_two, total_two = later
    top_new = jnp.maximum(total_two + top_one, top_two)
    scale_one = jnp.exp(total_two + top_one - top_new)
    scale_two = jnp.exp(top_two - top_new)
    state_new = scale_one[..., None, None] * state_one + scale_two[..., None, None] * state_two
    return (state_new, top_new, total_one + total_two)


def add_halves(kept, sent, axis, bit):
    received = swap(sent.astype(jnp.bfloat16), axis, bit)
    return kept.astype(jnp.float32) + received.astype(jnp.float32)


def layer(
    queries,
    key_head_rows,
    value_head_rows,
    output_gate_preact,
    log_input_gate,
    forget_gate_preact,
    extra_log_decay,
    head_norm_gain,
    residual,
    cell_output_weight,
    feedforward_norm_gain,
    gate_projection_weight,
    up_projection_weight,
    down_projection_weight,
):
    size = lax.axis_size("sp")
    here = lax.axis_index("sp")
    place = lax.axis_index("tp")
    tp_bits = bits_below(lax.axis_size("tp"))
    sp_bits = bits_below(size)
    share = sp_bits[len(sp_bits) // 2]
    others = [bit for bit in reversed(sp_bits) if bit != share]
    half = gate_projection_weight.shape[1] // 2
    upper = (here & share) != 0

    def halves(first, second):
        return jnp.where(upper, second, first), jnp.where(upper, first, second)

    def columns_of(weight):
        mine, theirs = halves(weight[:, :half], weight[:, half:])
        return jnp.concatenate(halves(mine, swap(theirs, "sp", share)), axis=0)

    def rows_of(weight):
        mine, theirs = halves(weight[:half], weight[half:])
        return jnp.concatenate(halves(mine, swap(theirs, "sp", share)), axis=1)

    gate_pair = columns_of(gate_projection_weight)
    up_pair = columns_of(up_projection_weight)
    down_pair = rows_of(down_projection_weight)
    gate_pieces = spread(gate_pair, others)
    up_pieces = spread(up_pair, others)
    down_pieces = spread(down_pair, others)

    tokens_here = queries.shape[0]
    heads_here = queries.shape[1] // DQK
    scale = DQK ** (-0.5)
    query_rows = queries.reshape(tokens_here, heads_here, DQK)
    key_rows = key_head_rows.reshape(tokens_here, heads_here, DQK)
    value_rows = value_head_rows.reshape(tokens_here, heads_here, DV)

    log_forget = jax.nn.log_sigmoid(forget_gate_preact) + extra_log_decay
    in_block = jnp.cumsum(log_forget.reshape(heads_here, -1, BLOCK), axis=-1)
    block_ends = jnp.cumsum(in_block[..., -1], axis=-1)
    block_starts = jnp.pad(block_ends[:, :-1], ((0, 0), (1, 0)))
    running = (in_block + block_starts[..., None]).reshape(heads_here, tokens_here)
    total = block_ends[:, -1]
    to_end = total[:, None] - running + log_input_gate
    top = jnp.max(to_end, axis=-1)
    factor = jnp.exp(to_end - top[:, None]) * scale
    weighted = (key_rows * factor.T[:, :, None]).astype(jnp.bfloat16)
    state = jnp.einsum("shd,she->hde", weighted, value_rows, preferred_element_type=jnp.float32)
    blank_state = (
        jnp.zeros((heads_here, DQK, DV), jnp.float32),
        jnp.full((heads_here,), lowest, jnp.float32),
        jnp.zeros((heads_here,), jnp.float32),
    )
    carried_state, carried_top, _ = prefix_of((state, top, total), "sp", blank_state)

    gain = log_input_gate - running
    causal = jnp.arange(tokens_here)[:, None] >= jnp.arange(tokens_here)[None, :]
    gain_seen = jnp.where(causal, gain[:, None, :], -jnp.inf)
    own_top = jnp.max(gain_seen, axis=-1)
    scores = (
        jnp.einsum("thd,shd->hts", query_rows, key_rows, preferred_element_type=jnp.float32)
        * scale
    )
    weights = (scores * jnp.exp(gain_seen - own_top[..., None])).astype(jnp.bfloat16)
    within = jnp.einsum("hts,she->hte", weights, value_rows, preferred_element_type=jnp.float32)
    across = jnp.einsum(
        "thd,hde->hte",
        query_rows.astype(jnp.float32),
        carried_state,
        precision=lax.Precision.HIGHEST,
    )
    row_top = jnp.maximum(carried_top[:, None], own_top)
    numerators = (
        jnp.exp(carried_top[:, None] - row_top)[..., None] * across
        + jnp.exp(own_top - row_top)[..., None] * within
    )
    normalized = numerators * lax.rsqrt(
        jnp.mean(numerators * numerators, axis=-1, keepdims=True) + epsilon
    )
    cell_rows = (
        normalized.transpose(1, 0, 2).reshape(tokens_here, heads_here * DV)
        * head_norm_gain
        * jax.nn.sigmoid(output_gate_preact.astype(jnp.float32))
    ).astype(jnp.bfloat16)

    tp_size = lax.axis_size("tp")
    rows = tokens_here // tp_size
    order = [0]
    for bit in reversed(tp_bits):
        order = order + [mask | bit for mask in order]

    def cell_product(some):
        left = jnp.concatenate(
            [lax.dynamic_slice_in_dim(cell_rows, (place ^ m) * rows, rows, 0) for m in some], axis=0
        )
        product = jnp.dot(left, cell_output_weight, preferred_element_type=jnp.float32)
        return product.astype(jnp.bfloat16)

    far = cell_product(order[tp_size // 2 :])
    projected = add_halves(cell_product(order[: tp_size // 2]), far, "tp", tp_bits[0])
    for bit in tp_bits[1:]:
        kept, sent = jnp.split(projected, 2, axis=0)
        projected = add_halves(kept.astype(jnp.bfloat16), sent, "tp", bit)
    mixed_float = (
        (residual.astype(jnp.float32) + projected).astype(jnp.bfloat16).astype(jnp.float32)
    )
    normed = (
        mixed_float
        * lax.rsqrt(jnp.mean(mixed_float * mixed_float, axis=-1, keepdims=True) + epsilon)
        * feedforward_norm_gain
    ).astype(jnp.bfloat16)

    early = [mask for mask, _ in gate_pieces if not mask & others[0]]
    late = [mask for mask, _ in gate_pieces if mask & others[0]]

    def joined(pieces, masks):
        return jnp.concatenate([dict(pieces)[mask] for mask in masks], axis=0)

    gate_early, up_early = joined(gate_pieces, early), joined(up_pieces, early)
    gate_late, up_late = joined(gate_pieces, late), joined(up_pieces, late)
    normed, gate_early = lax.optimization_barrier((normed, gate_early))

    width = gate_projection_weight.shape[0]
    base = here & ~share
    normed = jnp.concatenate(
        [
            lax.dynamic_slice_in_dim(normed, ((base ^ mask) | low) * width, width, 1)
            for mask in early + late
            for low in (0, share)
        ],
        axis=1,
    )
    paired = swap(normed, "sp", share)
    paired, up_early = lax.optimization_barrier((paired, up_early))
    held = [normed, paired]
    for bit in reversed(tp_bits[1:]):
        held = held + [swap(v, "tp", bit) for v in held]
    near_rows = jnp.concatenate(held, axis=0)
    far_rows = swap(near_rows, "tp", tp_bits[0])

    def product_of(left, first, second):
        split = first.shape[0]
        return jnp.dot(left[:, :split], first, preferred_element_type=jnp.float32) + jnp.dot(
            left[:, split:], second, preferred_element_type=jnp.float32
        )

    def hidden_of(left):
        gate_proj = product_of(left, gate_early, gate_late)
        up_proj = product_of(left, up_early, up_late)
        return (jax.nn.silu(gate_proj) * up_proj).astype(jnp.bfloat16)

    hidden_near = hidden_of(near_rows)
    hidden_far = hidden_of(far_rows)

    def down_product(left, piece):
        product = jnp.dot(left, piece, preferred_element_type=jnp.float32)
        return product.astype(jnp.bfloat16)

    def sum_pair(partial):
        parts = partial.reshape(-1, 2, rows, partial.shape[1])
        kept, sent = (parts[:, k].reshape(-1, partial.shape[1]) for k in (0, 1))
        return add_halves(kept, sent, "sp", share)

    def sum_rest(partial):
        for bit in tp_bits[1:]:
            kept, sent = jnp.split(partial.astype(jnp.bfloat16), 2, axis=0)
            partial = add_halves(kept, sent, "tp", bit)
        return partial

    blocks = {}
    for k, (mask, piece) in enumerate(sorted(down_pieces, key=lambda entry: entry[0])):
        far = down_product(hidden_far, piece)
        near = down_product(hidden_near, piece)
        partial = add_halves(near, far, "tp", tp_bits[0]).astype(jnp.bfloat16)
        if k % 2:
            blocks[mask] = sum_rest(sum_pair(partial))
        else:
            blocks[mask] = sum_pair(sum_rest(partial).astype(jnp.bfloat16))
    lows = share.bit_length() - 1
    masks = sorted(blocks)
    relative = jnp.concatenate([blocks[mask] for mask in masks], axis=1)
    columns = []
    for block in range(size):
        mask = (block ^ here) & ~share
        position = ((mask >> (lows + 1)) << lows) | (mask & (share - 1))
        start = (2 * position + ((block >> lows) & 1)) * width
        columns.append(lax.dynamic_slice_in_dim(relative, start, width, 1))
    summed = jnp.concatenate(columns, axis=1)
    return (mixed_float + summed).astype(jnp.bfloat16)


def solution(mesh):
    placed = (
        P("sp", "tp"),
        P("sp", "tp"),
        P("sp", "tp"),
        P("sp", "tp"),
        P("tp", "sp"),
        P("tp", "sp"),
        P("tp", "sp"),
        P("tp"),
        P(("sp", "tp"), None),
        P("tp", None),
        P(),
        P("sp", "tp"),
        P("sp", "tp"),
        P("tp", "sp"),
    )
    return jax.shard_map(
        layer, mesh=mesh, in_specs=placed, out_specs=P(("sp", "tp"), None), check_vma=False
    )
```
